32 devices in a mesh: sp: 8 (over z, y), dp: 4 (over x, core).
Axes of the slice: x: 2, y: 2, z: 4, core: 2. Of those that a mesh axis runs over, the one named last changes fastest.
Arguments:
- stream: bfloat16 [4, 1024, 2048], P('dp', 'sp'), may hold values from -6 to 6
- queries: bfloat16 [4, 1024, 1024], P('dp', 'sp'), may hold values from -6 to 6
- keys_in: bfloat16 [4, 1024, 1024], P('dp', 'sp'), may hold values from -6 to 6
- values_in: bfloat16 [4, 1024, 1024], P('dp', 'sp'), may hold values from -6 to 6
- key_shift: bfloat16 [4, 1024, 16], P('dp', 'sp'), may hold values from -8 to 16
- head_shift: float32 [16], replicated, may hold values from -16 to 0
- mix_gain: float32 [1024], replicated, may hold values from 0.1 to 1.9
- out_weight: bfloat16 [1024, 2048], replicated, may hold values from -0.1875 to 0.1875
- post_gain: float32 [2048], replicated, may hold values from 0.1 to 1.9
- route: int32 [4, 1024, 2], P('dp', 'sp'), may hold values from 0 to 31, as said below
- route_weight: float32 [4, 1024, 2], P('dp', 'sp'), may hold values from 0.25 to 1
- w_gate: bfloat16 [32, 2048, 1024], P(('sp', 'dp')), may hold values from -0.125 to 0.125
- w_up: bfloat16 [32, 2048, 1024], P(('sp', 'dp')), may hold values from -0.125 to 0.125
- w_down: bfloat16 [32, 1024, 2048], P(('sp', 'dp')), may hold values from -0.1875 to 0.1875
Outputs:
- result: bfloat16 [4, 1024, 2048], P('dp', 'sp')
The draws below stay inside these ranges and needn't reach their ends.
Inputs may be any that keep to these rules, and one draw needn't show every extreme that they name: `route`: each token names two different experts of one group (the group of expert e is e // 8). Of the 128 tokens of one device, each expert is named by at most 16; in every draw the 8 experts of one group are each named by exactly 16 tokens of every device.
All inputs are finite; a program needn't handle non-finite values.
Results may differ from the reference program's by a relative error of at most 0.0085.
Values may be sent and summed in bfloat16 or wider, within the bound.
No kernel may reach another device: no remote copies, remote signals or barrier semaphores. Data moves between devices by JAX's collectives and lax.ppermute only.
A program may use at most 128 MiB of HBM per device.

```python
import math
import jax
import jax.numpy as jnp
from jax import lax

D = 2048
HEADS = 16
HD = 64
F = 1024
GROUPS = 4
TOK_DEV = 128
SEQUENCE_LENGTH = 1024
SEQUENCE_COUNT = 4
EXPERTS = 32
EPG = 8
CAP = 16
N_SP = 8
N_DP = 4


def head_rates(key):
    base = jax.random.fold_in(key, 11)
    share = jax.random.uniform(base, (HEADS,), jnp.float32, 0.4, 1.4)
    return -share * math.log(SEQUENCE_LENGTH)


def draw_head_shift(key, part):
    return head_rates(key)


def draw_key_shift(key, part):
    decay_rates = head_rates(key)
    random_jitter = jnp.clip(0.7 * jax.random.normal(jax.random.fold_in(key, 12), (SEQUENCE_COUNT, SEQUENCE_LENGTH // TOK_DEV, TOK_DEV, HEADS), jnp.float32), -3.0, 3.0)
    offset = jax.random.uniform(jax.random.fold_in(key, 13), (SEQUENCE_COUNT, SEQUENCE_LENGTH // TOK_DEV, 1, HEADS), jnp.float32, -0.7, 0.7)
    random_jitter = (random_jitter + offset).reshape(SEQUENCE_COUNT, SEQUENCE_LENGTH, HEADS)
    sudden_spike = jax.random.randint(jax.random.fold_in(key, 14), (SEQUENCE_COUNT, SEQUENCE_LENGTH, 1), 0, max(SEQUENCE_LENGTH // 4, 2)) == 0
    value_entry = jnp.where(sudden_spike, -decay_rates[None, None, :] - 0.7, random_jitter)
    return value_entry.astype(jnp.bfloat16)


def draw_route(key, part):
    nblocks = SEQUENCE_COUNT * (SEQUENCE_LENGTH // TOK_DEV)
    half = TOK_DEV // 2
    hot = jax.random.randint(jax.random.fold_in(key, 21), (), 0, GROUPS)
    cuts = jnp.sort(jax.random.randint(jax.random.fold_in(key, 22), (nblocks, GROUPS - 2), 0, half + 1), axis=1)
    bounds = jnp.concatenate([jnp.zeros((nblocks, 1), jnp.int32), cuts, jnp.full((nblocks, 1), half, jnp.int32)], axis=1)
    others = bounds[:, 1:] - bounds[:, :-1]
    sizes = jnp.concatenate([jnp.full((nblocks, 1), half, jnp.int32), others], axis=1)
    ends = jnp.cumsum(sizes, axis=1)
    starts = ends - sizes
    position = jnp.arange(TOK_DEV, dtype=jnp.int32)
    section = jnp.sum((position[None, :, None] >= ends[:, None, :]).astype(jnp.int32), axis=2)
    within = position[None, :] - jnp.take_along_axis(starts, section, axis=1)
    group = (hot + section) % GROUPS
    per_row = EPG // 2
    row_idx = within // per_row
    col_idx = within % per_row
    scores = jax.random.randint(jax.random.fold_in(key, 23), (nblocks, GROUPS, CAP, EPG), 0, 2 ** 20) * EPG + jnp.arange(EPG, dtype=jnp.int32)
    perm = jnp.argsort(scores, axis=-1, stable=True).astype(jnp.int32).reshape(nblocks, GROUPS * CAP * EPG)
    flat_idx = (section * CAP + row_idx) * EPG + 2 * col_idx
    first = jnp.take_along_axis(perm, flat_idx, axis=1) + group * EPG
    second = jnp.take_along_axis(perm, flat_idx + 1, axis=1) + group * EPG
    pairs = jnp.stack([first, second], axis=2)
    tscore = jax.random.randint(jax.random.fold_in(key, 24), (nblocks, TOK_DEV), 0, 2 ** 20) * TOK_DEV + position[None, :]
    placement = jnp.argsort(tscore, axis=1, stable=True).astype(jnp.int32)
    shuffled = jnp.take_along_axis(pairs, placement[:, :, None], axis=1)
    return shuffled.reshape(SEQUENCE_COUNT, SEQUENCE_LENGTH, 2).astype(jnp.int32)


def steps_of(rng, dims, cuts, low, high):
    loudness, own = 1.0, jax.random.fold_in(rng, 6)
    for axis_at, blocks in cuts:
        heights = jnp.exp(jax.random.uniform(jax.random.fold_in(own, axis_at), (blocks,), jnp.float32, low / len(cuts), high / len(cuts)))
        loudness = loudness * jnp.repeat(heights, dims[axis_at] // blocks).reshape([-1 if axis == axis_at else 1 for axis in range(len(dims))])
    return loudness


def noise(key, dims, scale, most, cuts=(), kind=jnp.bfloat16):
    drawn = scale * jax.random.normal(key, dims, jnp.float32)
    if cuts:
        drawn = drawn * steps_of(key, dims, cuts, -0.22, 0.18)
    return jnp.clip(drawn, -most, most).astype(kind)


def setup_inputs(seed: int = 0) -> dict:
    arg_keys = jax.random.split(jax.random.key(seed), 15)
    stream = noise(arg_keys[0], (SEQUENCE_COUNT, SEQUENCE_LENGTH, D), 1.0, 6.0, ((0, 4), (1, 8)))
    queries = noise(arg_keys[1], (SEQUENCE_COUNT, SEQUENCE_LENGTH, HEADS * HD), 1.0, 6.0, ((0, 4), (1, 8)))
    keys_in = noise(arg_keys[2], (SEQUENCE_COUNT, SEQUENCE_LENGTH, HEADS * HD), 1.0, 6.0, ((0, 4), (1, 8)))
    values_in = noise(arg_keys[3], (SEQUENCE_COUNT, SEQUENCE_LENGTH, HEADS * HD), 1.0, 6.0, ((0, 4), (1, 8)))
    key_shift = draw_key_shift(jax.random.fold_in(arg_keys[14], 71), 0)
    head_shift = draw_head_shift(jax.random.fold_in(arg_keys[14], 71), 0)
    mix_gain = jnp.clip(1.0 + 0.18 * jax.random.normal(arg_keys[6], (HEADS * HD,), jnp.float32), 0.1, 1.9)
    out_weight = noise(arg_keys[7], (HEADS * HD, D), (HEADS * HD) ** -0.5, 0.1875)
    post_gain = jnp.clip(1.0 + 0.18 * jax.random.normal(arg_keys[8], (D,), jnp.float32), 0.1, 1.9)
    route = draw_route(jax.random.fold_in(arg_keys[14], 71), 0)
    route_weight = jnp.clip(jnp.exp(math.log(1.0) - 1.3862944 * jax.random.uniform(arg_keys[10], (SEQUENCE_COUNT, SEQUENCE_LENGTH, 2), jnp.float32) ** steps_of(arg_keys[10], (SEQUENCE_COUNT, SEQUENCE_LENGTH, 2), ((0, 4), (1, 8)), -0.2, 0.2)), 0.25, 1.0)
    w_gate = noise(arg_keys[11], (EXPERTS, D, F), D ** -0.5, 0.125, ((0, 32),))
    w_up = noise(arg_keys[12], (EXPERTS, D, F), D ** -0.5, 0.125, ((0, 32),))
    w_down = noise(arg_keys[13], (EXPERTS, F, D), F ** -0.5, 0.1875, ((0, 32),))
    return dict(stream=stream, queries=queries, keys_in=keys_in, values_in=values_in, key_shift=key_shift, head_shift=head_shift, mix_gain=mix_gain, out_weight=out_weight, post_gain=post_gain, route=route, route_weight=route_weight, w_gate=w_gate, w_up=w_up, w_down=w_down)


norm_eps = 1e-05

def block_total(length):
    blocks = 1
    while blocks * 2 <= min(8, length // 512):
        blocks = blocks * 2
    return blocks

def stick_head(queries_head, keys_head, values_head, offsets):
    length = queries_head.shape[0]
    blocks = block_total(length)
    width = length // blocks
    scale = 1.0 / math.sqrt(HD)
    pieces = []
    for block_idx in range(blocks):
        begin = block_idx * width
        finish = begin + width
        logits = jnp.dot(queries_head[begin:finish].astype(jnp.float32), keys_head[:finish].astype(jnp.float32).T, precision=lax.Precision.HIGHEST, preferred_element_type=jnp.float32) * scale
        logits = logits + offsets[None, :finish]
        rows_pos = begin + jnp.arange(width, dtype=jnp.int32)
        cols_pos = jnp.arange(finish, dtype=jnp.int32)
        causal = cols_pos[None, :] < rows_pos[:, None]
        breaks = jnp.where(causal, jax.nn.log_sigmoid(-logits), 0.0)
        suffix = lax.cumsum(breaks, axis=1, reverse=True) - breaks
        weights = jnp.where(causal, jnp.exp(jax.nn.log_sigmoid(logits) + suffix), 0.0).astype(jnp.bfloat16)
        pieces.append(jnp.dot(weights.astype(jnp.float32), values_head[:finish].astype(jnp.float32), precision=lax.Precision.HIGHEST, preferred_element_type=jnp.float32))
    return jnp.concatenate(pieces, axis=0)

def reference(stream, queries, keys_in, values_in, key_shift, head_shift, mix_gain, out_weight, post_gain, route, route_weight, w_gate, w_up, w_down):

    def by_head(array):
        return array.reshape(SEQUENCE_COUNT, SEQUENCE_LENGTH, HEADS, HD).transpose(0, 2, 1, 3).reshape(SEQUENCE_COUNT * HEADS, SEQUENCE_LENGTH, HD)
    offsets = key_shift.astype(jnp.float32).transpose(0, 2, 1) + head_shift[None, :, None]
    offsets = offsets.reshape(SEQUENCE_COUNT * HEADS, SEQUENCE_LENGTH)

    def one_head(items):
        return stick_head(items[0], items[1], items[2], items[3]).astype(jnp.bfloat16)
    attended = lax.map(one_head, (by_head(queries), by_head(keys_in), by_head(values_in), offsets))
    attended = attended.reshape(SEQUENCE_COUNT, HEADS, SEQUENCE_LENGTH, HD).transpose(0, 2, 1, 3).reshape(SEQUENCE_COUNT * SEQUENCE_LENGTH, HEADS * HD)
    att32 = attended.astype(jnp.float32)
    normed = (att32 * lax.rsqrt(lax.optimization_barrier(jnp.mean(att32 * att32, axis=1, keepdims=True)) + norm_eps) * mix_gain).astype(jnp.bfloat16)
    mixed = jnp.dot(normed.astype(jnp.float32), out_weight.astype(jnp.float32), precision=lax.Precision.HIGHEST, preferred_element_type=jnp.float32)
    summed = stream.reshape(SEQUENCE_COUNT * SEQUENCE_LENGTH, D).astype(jnp.float32) + mixed
    hidden = (summed * lax.rsqrt(lax.optimization_barrier(jnp.mean(summed * summed, axis=1, keepdims=True)) + norm_eps) * post_gain).astype(jnp.bfloat16)
    total = SEQUENCE_COUNT * SEQUENCE_LENGTH
    expert_ids = route.reshape(total * 2).astype(jnp.int32)
    weights_flat = route_weight.reshape(total * 2)
    order = jnp.argsort(expert_ids, stable=True).astype(jnp.int32)
    tok_sorted = order // 2
    weight_sorted = weights_flat[order]
    counts = lax.optimization_barrier(jnp.sum((expert_ids[:, None] == jnp.arange(EXPERTS, dtype=jnp.int32)[None, :]).astype(jnp.int32), axis=0))
    starts = (jnp.cumsum(counts) - counts).astype(jnp.int32)
    most_rows = N_SP * N_DP * CAP
    tok_padded = jnp.concatenate([tok_sorted, jnp.zeros((most_rows,), jnp.int32)])
    weight_padded = jnp.concatenate([weight_sorted, jnp.zeros((most_rows,), jnp.float32)])

    def one_expert(carry, expert):
        index_rows = lax.dynamic_slice(tok_padded, (starts[expert],), (most_rows,))
        weight_rows = lax.dynamic_slice(weight_padded, (starts[expert],), (most_rows,))
        valid = jnp.arange(most_rows, dtype=jnp.int32) < counts[expert]
        rows = hidden[index_rows].astype(jnp.float32)
        gate = jnp.dot(rows, w_gate[expert].astype(jnp.float32), precision=lax.Precision.HIGHEST, preferred_element_type=jnp.float32)
        upper = jnp.dot(rows, w_up[expert].astype(jnp.float32), precision=lax.Precision.HIGHEST, preferred_element_type=jnp.float32)
        inner = (jax.nn.silu(gate) * upper).astype(jnp.bfloat16)
        output = jnp.dot(inner.astype(jnp.float32), w_down[expert].astype(jnp.float32), precision=lax.Precision.HIGHEST, preferred_element_type=jnp.float32).astype(jnp.bfloat16)
        scaled_values = jnp.where(valid[:, None], weight_rows[:, None] * output.astype(jnp.float32), 0.0)
        return (carry.at[index_rows].add(scaled_values), None)
    moe_sum, _ = lax.scan(one_expert, jnp.zeros((total, D), jnp.float32), jnp.arange(EXPERTS, dtype=jnp.int32))
    result = (hidden.astype(jnp.float32) + moe_sum).astype(jnp.bfloat16)
    return result.reshape(SEQUENCE_COUNT, SEQUENCE_LENGTH, D)
```

```python
import functools
import math

import jax
import jax.numpy as jnp
from jax import lax
from jax.experimental import pallas as pl
from jax.experimental.pallas import tpu as pltpu
from jax.sharding import PartitionSpec as P

HD = 64
GROUPS = 4
norm_eps = 1e-05
F32 = jnp.float32
BF16 = jnp.bfloat16
MB = 1024 * 1024

VM = pl.BlockSpec(memory_space=pltpu.VMEM)
SM = pl.BlockSpec(memory_space=pltpu.SMEM)
NT = (((1,), (1,)), ((), ()))


def call(body, out, n_in, scratch=(), limit=40, in_specs=None, flops=0, name=None):
    return pl.pallas_call(
        body,
        out_shape=out,
        in_specs=in_specs or [VM] * n_in,
        out_specs=jax.tree.map(lambda _: VM, out),
        scratch_shapes=list(scratch),
        compiler_params=pltpu.CompilerParams(vmem_limit_bytes=limit * MB),
        cost_estimate=pl.CostEstimate(flops=flops, bytes_accessed=MB, transcendentals=0),
        name=name,
    )


def iota(shape, dim):
    return lax.broadcasted_iota(jnp.int32, shape, dim)


def pack_body(q_ref, k_ref, v_ref, ks_ref, out_ref):
    n, rows, cols = out_ref.shape
    tokens, heads = ks_ref.shape[1], ks_ref.shape[2]
    local = heads // n
    pieces = tokens // cols
    eye = (iota((heads, heads), 0) == iota((heads, heads), 1)).astype(BF16)
    shift = lax.dot_general(eye, ks_ref[0], NT, preferred_element_type=F32)
    pad = rows - 3 * tokens
    for d in range(n):
        lanes = slice(d * cols, (d + 1) * cols)
        out_ref[d, 0:tokens, :] = q_ref[0, :, lanes]
        out_ref[d, tokens : 2 * tokens, :] = k_ref[0, :, lanes]
        out_ref[d, 2 * tokens : 3 * tokens, :] = v_ref[0, :, lanes]
        tail = [
            shift[d * local + h : d * local + h + 1, p * cols : (p + 1) * cols]
            for h in range(local)
            for p in range(pieces)
        ]
        tail.append(jnp.zeros((pad - len(tail), cols), F32))
        out_ref[d, 3 * tokens :, :] = jnp.concatenate(tail, axis=0).astype(BF16)


def attention_body(hs_ref, x_ref, out_ref, z_ref, w_ref):
    n, _, cols = x_ref.shape
    tokens = out_ref.shape[1]
    local = cols // HD
    pieces = tokens // cols
    lane = iota((tokens, cols), 1) // HD
    keys = x_ref[:, tokens : 2 * tokens, :].reshape(n * tokens, cols)
    values = x_ref[:, 2 * tokens : 3 * tokens, :].reshape(n * tokens, cols)
    row, col = iota((2 * tokens, 2 * tokens), 0), iota((2 * tokens, 2 * tokens), 1)
    summing = jnp.where((col >= tokens) | (row % tokens >= col), 1.0, 0.0).astype(BF16)
    causal = iota((tokens, tokens), 1) < iota((tokens, tokens), 0)
    for i in range(n):
        total = None
        for h in range(local):
            q = x_ref[i, 0:tokens, :].astype(F32) * (1.0 / math.sqrt(HD))
            q = jnp.where(lane == h, q, 0.0).astype(BF16)
            span = (i + 1) * tokens
            z_ref[h, :, 0:span] = lax.dot_general(
                q, keys[0:span], NT, preferred_element_type=F32
            )
            carry = None
            for j in range(i, -1, -1):
                at = slice(j * tokens, (j + 1) * tokens)
                base = 3 * tokens + h * pieces
                off = [x_ref[j, base + p : base + p + 1, :] for p in range(pieces)]
                off = off[0] if pieces == 1 else jnp.concatenate(off, axis=1)
                z = z_ref[h, :, at] + (off.astype(F32) + hs_ref[h])
                breaks = -(jnp.maximum(z, 0.0) + jnp.log(1.0 + jnp.exp(-jnp.abs(z))))
                if j == i:
                    breaks = jnp.where(causal, breaks, 0.0)
                high = breaks.astype(BF16)
                low = (breaks - high.astype(F32)).astype(BF16)
                sums = jnp.dot(
                    jnp.concatenate([high, low], axis=1), summing, preferred_element_type=F32
                )
                power = z + sums[:, 0:tokens]
                if carry is not None:
                    power = power + carry
                weight = jnp.exp(power)
                if j == i:
                    weight = jnp.where(causal, weight, 0.0)
                w_ref[h, :, at] = weight.astype(BF16)
                part = sums[:, tokens:]
                carry = part if carry is None else carry + part
            got = jnp.dot(w_ref[h, :, 0:span], values[0:span], preferred_element_type=F32)
            total = got if total is None else jnp.where(lane == h, got, total)
        out_ref[i] = total.astype(BF16)


def route_body(route_ref, row_ref, col_ref, *, n_expert, capacity):
    tokens = route_ref.shape[1]
    ids = route_ref[0].astype(F32)
    eye = iota((tokens, tokens), 0) == iota((tokens, tokens), 1)
    before = (iota((tokens, tokens), 0) < iota((tokens, tokens), 1)).astype(BF16)
    e_rows = [
        jnp.sum(jnp.where(eye, ids[:, k : k + 1], 0.0), axis=0, keepdims=True) for k in range(2)
    ]
    names = iota((n_expert, tokens), 0).astype(F32)
    hot = [(names == e).astype(F32) for e in e_rows]
    earlier = jnp.dot((hot[0] + hot[1]).astype(BF16), before, preferred_element_type=F32)
    rows, cols = [], []
    for k in range(2):
        rank = jnp.sum(hot[k] * earlier, axis=0, keepdims=True)
        dest = e_rows[k] * capacity + rank
        rows.append(dest)
        cols.append(jnp.sum(jnp.where(eye, dest, 0.0), axis=1, keepdims=True))
    row_ref[...] = jnp.concatenate(rows + [jnp.zeros((6, tokens), F32)], axis=0).astype(jnp.int32)
    lane = iota((tokens, 128), 1)
    col_ref[...] = jnp.where(lane == 0, cols[0], cols[1]).astype(jnp.int32)


def hidden_body(att_ref, stream_ref, mg_ref, w_ref, pg_ref, dest_ref, hid_ref, send_ref):
    n, tokens, cols = att_ref.shape
    pieces = [att_ref[s].astype(F32) for s in range(n)]
    if cols % 128 == 0:
        pieces = [jnp.concatenate(pieces, axis=1)]
    size = pieces[0].shape[1]
    square = sum(jnp.sum(p * p, axis=1, keepdims=True) for p in pieces)
    scale = lax.rsqrt(square / (n * cols) + norm_eps)
    mixed = None
    for s, p in enumerate(pieces):
        at = slice(s * size, (s + 1) * size)
        normed = (p * scale * mg_ref[:, at]).astype(BF16)
        part = jnp.dot(normed, w_ref[at, :], preferred_element_type=F32)
        mixed = part if mixed is None else mixed + part
    summed = stream_ref[0].astype(F32) + mixed
    mean = jnp.mean(summed * summed, axis=1, keepdims=True)
    hidden = (summed * lax.rsqrt(mean + norm_eps) * pg_ref[...]).astype(BF16)
    hid_ref[...] = hidden
    total = send_ref.shape[0]
    slot = iota((total, tokens), 0)
    pick = (slot == dest_ref[0:1, :]) | (slot == dest_ref[1:2, :])
    send_ref[...] = jnp.dot(
        pick.astype(F32).astype(BF16), hidden, preferred_element_type=F32
    ).astype(BF16)


def expert_body(x_ref, wg_ref, wu_ref, wd_ref, out_ref, acc_ref):
    step = pl.program_id(0)
    x = x_ref[...]
    gate = jnp.dot(x, wg_ref[0], preferred_element_type=F32)
    upper = jnp.dot(x, wu_ref[0], preferred_element_type=F32)
    inner = (gate / (1.0 + jnp.exp(-gate)) * upper).astype(BF16)
    part = jnp.dot(inner, wd_ref[0], preferred_element_type=F32)

    @pl.when(step == 0)
    def _():
        acc_ref[...] = part

    @pl.when(step > 0)
    def _():
        acc_ref[...] += part

    @pl.when(step == pl.num_programs(0) - 1)
    def _():
        out_ref[...] = acc_ref[...].astype(BF16)


def combine_body(ret_ref, hid_ref, rw_ref, dest_ref, out_ref):
    tokens = hid_ref.shape[0]
    total = ret_ref.shape[0]
    slot = iota((tokens, total), 1)
    result = hid_ref[...].astype(F32)
    for k in range(2):
        pick = (slot == dest_ref[:, k : k + 1]).astype(F32).astype(BF16)
        rows = jnp.dot(pick, ret_ref[...], preferred_element_type=F32)
        result = result + rows * rw_ref[0, :, k : k + 1]
    out_ref[0] = result.astype(BF16)


def on_device(
    stream,
    queries,
    keys_in,
    values_in,
    key_shift,
    head_shift,
    mix_gain,
    out_weight,
    post_gain,
    route,
    route_weight,
    w_gate,
    w_up,
    w_down,
):
    tokens, width = stream.shape[1], stream.shape[2]
    size_sp, size_dp = lax.axis_size("sp"), lax.axis_size("dp")
    heads = key_shift.shape[2]
    local = heads // size_sp
    cols = queries.shape[2] // size_sp
    rows = 3 * tokens + 16
    n_expert = size_sp * size_dp
    capacity = tokens // (n_expert // GROUPS)
    slots = n_expert * capacity
    sds = jax.ShapeDtypeStruct

    sent = call(pack_body, sds((size_sp, rows, cols), BF16), 4, name="pack")(
        queries, keys_in, values_in, key_shift
    )
    got = lax.all_to_all(sent, "sp", split_axis=0, concat_axis=0, tiled=True)
    dest_rows, dest_cols = call(
        functools.partial(route_body, n_expert=n_expert, capacity=capacity),
        (sds((8, tokens), jnp.int32), sds((tokens, 128), jnp.int32)),
        1,
        name="route",
    )(route)
    own_shift = lax.dynamic_slice_in_dim(head_shift, lax.axis_index("sp") * local, local)
    seq = size_sp * tokens
    att = call(
        attention_body,
        sds((size_sp, tokens, cols), BF16),
        2,
        in_specs=[SM, VM],
        scratch=[pltpu.VMEM((local, tokens, seq), F32), pltpu.VMEM((local, tokens, seq), BF16)],
        name="attention",
    )(own_shift, got)
    att = lax.all_to_all(att, "sp", split_axis=0, concat_axis=0, tiled=True)
    hidden, send = call(
        hidden_body,
        (sds((tokens, width), BF16), sds((slots, width), BF16)),
        6,
        name="hidden",
    )(att, stream, mix_gain[None], out_weight, post_gain[None], dest_rows)
    received = lax.all_to_all(
        send.reshape(n_expert, capacity, width),
        ("sp", "dp"),
        split_axis=0,
        concat_axis=0,
        tiled=True,
    ).reshape(slots, width)
    f = w_gate.shape[2]
    step = min(256, f)
    reply = pl.pallas_call(
        expert_body,
        grid=(f // step,),
        out_shape=sds((slots, width), BF16),
        in_specs=[
            pl.BlockSpec((slots, width), lambda s: (0, 0)),
            pl.BlockSpec((1, width, step), lambda s: (0, 0, s)),
            pl.BlockSpec((1, width, step), lambda s: (0, 0, s)),
            pl.BlockSpec((1, step, width), lambda s: (0, s, 0)),
        ],
        out_specs=pl.BlockSpec((slots, width), lambda s: (0, 0)),
        scratch_shapes=[pltpu.VMEM((slots, width), F32)],
        compiler_params=pltpu.CompilerParams(vmem_limit_bytes=48 * MB),
        name="experts",
    )(received, w_gate, w_up, w_down)
    returned = lax.all_to_all(
        reply.reshape(n_expert, capacity, width),
        ("sp", "dp"),
        split_axis=0,
        concat_axis=0,
        tiled=True,
    ).reshape(slots, width)
    return call(combine_body, sds((1, tokens, width), BF16), 4, name="combine")(
        returned, hidden, route_weight, dest_cols
    )


def solution(mesh):
    return jax.shard_map(
        on_device,
        mesh=mesh,
        in_specs=(
            P("dp", "sp", None),
            P("dp", "sp", None),
            P("dp", "sp", None),
            P("dp", "sp", None),
            P("dp", "sp", None),
            P(),
            P(),
            P(),
            P(),
            P("dp", "sp", None),
            P("dp", "sp", None),
            P(("sp", "dp"), None, None),
            P(("sp", "dp"), None, None),
            P(("sp", "dp"), None, None),
        ),
        out_specs=P("dp", "sp", None),
        check_vma=False,
    )
```

```python
import functools
import math

import jax
import jax.numpy as jnp
from jax import lax
from jax.experimental import pallas as pl
from jax.experimental.pallas import tpu as pltpu
from jax.sharding import PartitionSpec as P


HD = 64
GROUPS = 4
CORES = 2
CHUNKS = ((2,), (3,), (0, 1))
norm_eps = 1e-05
F32 = jnp.float32
BF16 = jnp.bfloat16
MB = 1024 * 1024
FLOPS = 1.5e7
BYTES = 3.0e6

VM = pl.BlockSpec(memory_space=pltpu.VMEM)
SM = pl.BlockSpec(memory_space=pltpu.SMEM)
NT = (((1,), (1,)), ((), ()))


def call(body, out, n_in, scratch=(), limit=8, in_specs=None, us=1.0):
    return pl.pallas_call(
        body,
        out_shape=out,
        in_specs=in_specs or [VM] * n_in,
        out_specs=jax.tree.map(lambda _: VM, out),
        scratch_shapes=list(scratch),
        compiler_params=pltpu.CompilerParams(vmem_limit_bytes=limit * MB),
        cost_estimate=pl.CostEstimate(flops=int(us * FLOPS), bytes_accessed=int(us * BYTES), transcendentals=0),
    )


def iota(shape, dim):
    return lax.broadcasted_iota(jnp.int32, shape, dim)


def pack_body(q_ref, k_ref, v_ref, ks_ref, out_ref):
    n, rows, cols = out_ref.shape
    tokens, heads = ks_ref.shape[1], ks_ref.shape[2]
    local = heads // n
    pieces = tokens // cols
    eye = (iota((heads, heads), 0) == iota((heads, heads), 1)).astype(BF16)
    shift = lax.dot_general(eye, ks_ref[0], NT, preferred_element_type=F32)
    pad = rows - 3 * tokens
    for d in range(n):
        lanes = slice(d * cols, (d + 1) * cols)
        out_ref[d, 0:tokens, :] = q_ref[0, :, lanes]
        out_ref[d, tokens : 2 * tokens, :] = k_ref[0, :, lanes]
        out_ref[d, 2 * tokens : 3 * tokens, :] = v_ref[0, :, lanes]
        tail = [
            shift[d * local + h : d * local + h + 1, p * cols : (p + 1) * cols]
            for h in range(local)
            for p in range(pieces)
        ]
        tail.append(jnp.zeros((pad - len(tail), cols), F32))
        out_ref[d, 3 * tokens :, :] = jnp.concatenate(tail, axis=0).astype(BF16)


def pick_body(me_ref, q_ref, k_ref, v_ref, ks_ref, *out_refs):
    rows, cols = out_refs[0].shape
    tokens, heads = ks_ref.shape[1], ks_ref.shape[2]
    local = heads // len(out_refs)
    pad = rows - 3 * tokens
    line, head = iota((pad, heads), 0), iota((pad, heads), 1)
    for k, out_ref in enumerate(out_refs):
        target = me_ref[1] ^ k
        lanes = pl.ds(pl.multiple_of(target * cols, cols), cols)
        out_ref[0:tokens, :] = q_ref[0, :, lanes]
        out_ref[tokens : 2 * tokens, :] = k_ref[0, :, lanes]
        out_ref[2 * tokens : 3 * tokens, :] = v_ref[0, :, lanes]
        take = ((head == line + target * local) & (line < local)).astype(F32).astype(BF16)
        out_ref[3 * tokens :, :] = lax.dot_general(
            take, ks_ref[0], NT, preferred_element_type=F32
        ).astype(BF16)


def attention_body(me_ref, hs_ref, *refs, fetches):
    n = (len(refs) - 5 - 2 * fetches)
    x_refs, refs = refs[:n], refs[n:]
    sources, (out_ref, *kept), (x_ref, z_ref, w_ref, sems) = (
        refs[:fetches],
        refs[fetches : 2 * fetches + 1],
        refs[2 * fetches + 1 :],
    )
    copies = [
        pltpu.make_async_copy(source, target, sems.at[i])
        for i, (source, target) in enumerate(zip(sources, kept))
    ]
    for copy in copies:
        copy.start()
    for k, ref in enumerate(x_refs):
        x_ref[me_ref[1] ^ k] = ref[...]
    n, _, cols = x_ref.shape
    tokens = out_ref.shape[1]
    local = cols // HD
    pieces = tokens // cols
    lane = iota((tokens, cols), 1) // HD
    keys = x_ref[:, tokens : 2 * tokens, :].reshape(n * tokens, cols)
    values = x_ref[:, 2 * tokens : 3 * tokens, :].reshape(n * tokens, cols)
    row, col = iota((2 * tokens, 2 * tokens), 0), iota((2 * tokens, 2 * tokens), 1)
    summing = jnp.where((col >= tokens) | (row % tokens >= col), 1.0, 0.0).astype(BF16)
    causal = iota((tokens, tokens), 1) < iota((tokens, tokens), 0)
    for i in range(n):
        total = None
        for h in range(local):
            q = x_ref[i, 0:tokens, :].astype(F32) * (1.0 / math.sqrt(HD))
            q = jnp.where(lane == h, q, 0.0).astype(BF16)
            span = (i + 1) * tokens
            z_ref[h, :, 0:span] = lax.dot_general(
                q, keys[0:span], NT, preferred_element_type=F32
            )
            carry = None
            for j in range(i, -1, -1):
                at = slice(j * tokens, (j + 1) * tokens)
                base = 3 * tokens + h * pieces
                off = [x_ref[j, base + p : base + p + 1, :] for p in range(pieces)]
                off = off[0] if pieces == 1 else jnp.concatenate(off, axis=1)
                z = z_ref[h, :, at] + (off.astype(F32) + hs_ref[me_ref[1] * local + h])
                breaks = -(jnp.maximum(z, 0.0) + jnp.log(1.0 + jnp.exp(-jnp.abs(z))))
                if j == i:
                    breaks = jnp.where(causal, breaks, 0.0)
                high = breaks.astype(BF16)
                low = (breaks - high.astype(F32)).astype(BF16)
                sums = jnp.dot(
                    jnp.concatenate([high, low], axis=1), summing, preferred_element_type=F32
                )
                power = z + sums[:, 0:tokens]
                if carry is not None:
                    power = power + carry
                weight = jnp.exp(power)
                if j == i:
                    weight = jnp.where(causal, weight, 0.0)
                w_ref[h, :, at] = weight.astype(BF16)
                part = sums[:, tokens:]
                carry = part if carry is None else carry + part
            got = jnp.dot(w_ref[h, :, 0:span], values[0:span], preferred_element_type=F32)
            total = got if total is None else jnp.where(lane == h, got, total)
        out_ref[i] = total.astype(BF16)
    for copy in copies:
        copy.wait()


def route_body(me_ref, route_ref, rw_ref, row_ref, col_ref, *meta_refs, plane, cap):
    tokens = route_ref.shape[1]
    bits = plane.bit_length() - 1
    zme, pme = me_ref[0] >> bits, me_ref[0] & (plane - 1)
    ids = route_ref[0].astype(F32)
    eye = iota((tokens, tokens), 0) == iota((tokens, tokens), 1)
    before = (iota((tokens, tokens), 0) < iota((tokens, tokens), 1)).astype(BF16)

    def to_row(col):
        return jnp.sum(jnp.where(eye, col, 0.0), axis=0, keepdims=True)

    def to_col(row):
        return jnp.sum(jnp.where(eye, row, 0.0), axis=1, keepdims=True)

    def count(hot):
        return jnp.dot(hot.astype(BF16), before, preferred_element_type=F32)

    e_rows = [to_row(ids[:, k : k + 1]) for k in range(2)]
    names = iota((GROUPS * plane, tokens), 0).astype(F32)
    hot = [(names == e).astype(F32) for e in e_rows]
    earlier = count(hot[0] + hot[1])
    ranks = [jnp.sum(h * earlier, axis=0, keepdims=True) for h in hot]
    group = e_rows[0].astype(jnp.int32) >> bits
    in_group = (iota((8, tokens), 0) == group).astype(F32)
    place = jnp.sum(in_group * count(in_group), axis=0, keepdims=True)
    spot = [e.astype(jnp.int32) & (plane - 1) for e in e_rows]
    rows = [jnp.where(group == (zme ^ d), place, -1.0) for d in range(GROUPS)]
    row_ref[...] = jnp.concatenate(rows + [jnp.zeros((4, tokens), F32)], axis=0).astype(jnp.int32)
    lane = iota((tokens, 128), 1)
    cols = [to_col(r) for r in rows]
    table = jnp.zeros((tokens, 128), F32)
    for k, c in enumerate(cols):
        table = jnp.where(lane == k, c, table)
    col_ref[...] = table.astype(jnp.int32)
    offset = [(p ^ pme) for p in spot]
    slot = iota((tokens, tokens), 1).astype(F32)
    for d, (c, ref) in enumerate(zip(cols, meta_refs)):
        chunk = next(chunk for chunk in CHUNKS if d in chunk)
        sources, source = len(chunk), chunk.index(d)
        relay = [
            to_col(((q * sources + source) * cap).astype(F32) + r) for q, r in zip(offset, ranks)
        ]
        pick = slot == c
        out = [
            jnp.sum(jnp.where(pick, v + 1.0, 0.0), axis=0, keepdims=True) - 1.0 for v in relay
        ]
        out += [
            jnp.sum(jnp.where(pick, rw_ref[0, :, k : k + 1], 0.0), axis=0, keepdims=True)
            for k in range(2)
        ]
        ref[...] = jnp.concatenate(out + [jnp.zeros((4, tokens), F32)], axis=0)


def hidden_body(att_ref, stream_ref, mg_ref, w_ref, pg_ref, dest_ref, hid_ref, *far_refs):
    n, tokens, cols = att_ref.shape
    pieces = [att_ref[s].astype(F32) for s in range(n)]
    if cols % 128 == 0:
        pieces = [jnp.concatenate(pieces, axis=1)]
    size = pieces[0].shape[1]
    square = sum(jnp.sum(p * p, axis=1, keepdims=True) for p in pieces)
    scale = lax.rsqrt(square / (n * cols) + norm_eps)
    mixed = None
    for s, p in enumerate(pieces):
        at = slice(s * size, (s + 1) * size)
        normed = (p * scale * mg_ref[:, at]).astype(BF16)
        part = jnp.dot(normed, w_ref[at, :], preferred_element_type=F32)
        mixed = part if mixed is None else mixed + part
    summed = stream_ref[0].astype(F32) + mixed
    mean = jnp.mean(summed * summed, axis=1, keepdims=True)
    hidden = (summed * lax.rsqrt(mean + norm_eps) * pg_ref[...]).astype(BF16)
    hid_ref[...] = hidden
    for d, ref in enumerate(far_refs):
        pick = iota((ref.shape[0], tokens), 0) == dest_ref[d : d + 1, :]
        ref[...] = jnp.dot(
            pick.astype(F32).astype(BF16), hidden, preferred_element_type=F32
        ).astype(BF16)


def relay_body(*refs, sources):
    x_refs, meta_refs, out_refs = refs[:sources], refs[sources : 2 * sources], refs[2 * sources :]
    half = x_refs[0].shape[0]
    block = out_refs[0].shape[0]
    slot = iota((block * len(out_refs), half), 0)
    rows = None
    for x_ref, meta_ref in zip(x_refs, meta_refs):
        place = meta_ref[0:2, 0:half].astype(jnp.int32)
        pick = (slot == place[0:1]) | (slot == place[1:2])
        part = jnp.dot(pick.astype(F32).astype(BF16), x_ref[...], preferred_element_type=F32)
        rows = part if rows is None else rows + part
    rows = rows.astype(BF16)
    for m, ref in enumerate(out_refs):
        ref[...] = rows[m * block : (m + 1) * block]


def expert_body(*refs, takes):
    x_refs, (wg_ref, wu_ref, wd_ref), out_refs = (
        refs[: len(takes)],
        refs[len(takes) : len(takes) + 3],
        refs[len(takes) + 3 :],
    )
    parts = [ref[0:take] for ref, take in zip(x_refs, takes)]
    x = parts[0] if len(parts) == 1 else jnp.concatenate(parts, axis=0)
    gate = jnp.dot(x, wg_ref[0], preferred_element_type=F32)
    upper = jnp.dot(x, wu_ref[0], preferred_element_type=F32)
    inner = (gate / (1.0 + jnp.exp(-gate)) * upper).astype(BF16)
    out = jnp.dot(inner, wd_ref[0], preferred_element_type=F32).astype(BF16)
    at = 0
    for ref in out_refs:
        ref[...] = out[at : at + ref.shape[0]]
        at += ref.shape[0]


def second_halves_body(*refs):
    out_ref = refs[-1]
    part = out_ref.shape[0] // (len(refs) - 1)
    for m, ref in enumerate(refs[:-1]):
        out_ref[m * part : (m + 1) * part] = ref[part:]


def join_body(own_ref, back_ref, *out_refs):
    part = out_refs[0].shape[0] // 2
    for m, ref in enumerate(out_refs):
        at = slice(m * part, (m + 1) * part)
        ref[0:part] = own_ref[at]
        ref[part:] = back_ref[at]


def gather_body(*refs, sources):
    meta_refs, row_refs, out_refs = refs[:sources], refs[sources:-sources], refs[-sources:]
    parts = [ref[...] for ref in row_refs]
    rows = parts[0] if len(parts) == 1 else jnp.concatenate(parts, axis=0)
    for meta_ref, out_ref in zip(meta_refs, out_refs):
        half = out_ref.shape[0]
        eye = iota((half, half), 0) == iota((half, half), 1)
        slot = iota((half, rows.shape[0]), 1).astype(F32)
        total = None
        for k in range(2):
            place, weight = [
                jnp.sum(jnp.where(eye, meta_ref[r : r + 1, 0:half], 0.0), axis=1, keepdims=True)
                for r in (k, 2 + k)
            ]
            pick = (slot == place).astype(F32).astype(BF16)
            part = jnp.dot(pick, rows, preferred_element_type=F32) * weight
            total = part if total is None else total + part
        out_ref[...] = total.astype(BF16)


def combine_body(*refs):
    far_refs, (hid_ref, dest_ref, out_ref) = refs[:-3], refs[-3:]
    tokens = hid_ref.shape[0]
    result = hid_ref[...].astype(F32)
    for d, ref in enumerate(far_refs):
        slot = iota((tokens, ref.shape[0]), 1)
        hot = (slot == dest_ref[:, d : d + 1]).astype(F32).astype(BF16)
        result = result + jnp.dot(hot, ref[...], preferred_element_type=F32)
    out_ref[0] = result.astype(BF16)


def on_device(
    stream,
    queries,
    keys_in,
    values_in,
    key_shift,
    head_shift,
    mix_gain,
    out_weight,
    post_gain,
    route,
    route_weight,
    w_gate,
    w_up,
    w_down,
):
    tokens, width = stream.shape[1], stream.shape[2]
    size_sp, size_dp = lax.axis_size("sp"), lax.axis_size("dp")
    heads = key_shift.shape[2]
    local = heads // size_sp
    cols = queries.shape[2] // size_sp
    rows = 3 * tokens + 16
    n_expert = size_sp * size_dp
    plane = n_expert // GROUPS
    chips = plane // CORES
    cap = tokens // plane
    half = tokens // 2
    both = ("sp", "dp")
    sds = jax.ShapeDtypeStruct
    sp = lax.axis_index("sp")
    me = jnp.stack([sp * size_dp + lax.axis_index("dp"), sp]).astype(jnp.int32)

    def swap(array, bit):
        return lax.ppermute(array, both, [(i, i ^ bit) for i in range(n_expert)])

    if cols == tokens:
        sent = call(
            pick_body, (sds((rows, cols), BF16),) * size_sp, 5, in_specs=[SM, VM, VM, VM, VM]
        )(me, queries, keys_in, values_in, key_shift)
    else:
        sent = call(pack_body, sds((size_sp, rows, cols), BF16), 4)(
            queries, keys_in, values_in, key_shift
        )
        sent = [
            lax.dynamic_index_in_dim(sent, sp ^ k, 0, keepdims=False) for k in range(size_sp)
        ]
    got = [sent[0]] + [None] * (size_sp - 1)
    for k in range(size_sp - 1, 0, -1):
        got[k] = swap(sent[k], k * size_dp)
    dest_rows, dest_cols, *metas = call(
        functools.partial(route_body, plane=plane, cap=cap),
        (sds((8, tokens), jnp.int32), sds((tokens, 128), jnp.int32))
        + (sds((8, tokens), F32),) * GROUPS,
        3,
        in_specs=[SM, VM, VM],
    )(me, route, route_weight)
    metas = [metas[0]] + [swap(metas[d], d * plane) for d in range(1, GROUPS)]
    got, metas = lax.optimization_barrier((got, metas))
    seq = size_sp * tokens
    later = [
        pltpu.with_memory_space_constraint(array, pltpu.HBM)
        for array in (out_weight, stream, mix_gain[None], post_gain[None], w_down)
    ]
    att, out_weight, stream, mix_gain, post_gain, w_down = call(
        functools.partial(attention_body, fetches=len(later)),
        (sds((size_sp, tokens, cols), BF16),) + tuple(sds(x.shape, x.dtype) for x in later),
        0,
        in_specs=[SM, SM]
        + [VM] * size_sp
        + [pl.BlockSpec(memory_space=pltpu.HBM)] * len(later),
        scratch=[
            pltpu.VMEM((size_sp, rows, cols), BF16),
            pltpu.VMEM((local, tokens, seq), F32),
            pltpu.VMEM((local, tokens, seq), BF16),
            pltpu.SemaphoreType.DMA((len(later),)),
        ],
        us=8,
    )(me, head_shift, *got, *later)
    att = lax.all_to_all(att, "sp", split_axis=0, concat_axis=0, tiled=True)
    row = lambda count: sds((count, width), BF16)
    hidden, *far = call(
        hidden_body, (row(tokens),) + (row(half),) * GROUPS, 6, us=2
    )(att, stream, mix_gain, out_weight, post_gain, dest_rows)
    for d in range(1, GROUPS):
        far[d] = swap(far[d], d * plane)

    def experts(pieces, takes, outs):
        if any(take % 8 for take in takes):
            pieces = [jnp.concatenate([p[:t] for p, t in zip(pieces, takes)], axis=0)]
            takes = [sum(takes)]
        return call(
            functools.partial(expert_body, takes=takes),
            tuple(row(o) for o in outs),
            len(takes) + 3,
            limit=8,
            us=0.02 * sum(takes),
        )(*pieces, w_gate, w_up, w_down)

    sums = [None] * GROUPS
    for chunk in CHUNKS:
        sources = len(chunk)
        block = row(CORES * cap * sources)
        part = cap * sources
        blocks = call(
            functools.partial(relay_body, sources=sources), (block,) * chips, 2 * sources
        )(*[far[d] for d in chunk], *[metas[d] for d in chunk])
        held = [blocks[0]] + [swap(blocks[m], CORES * m) for m in range(1, chips)]
        if part % 16:
            other = jnp.concatenate([b[part:] for b in held], axis=0)
        else:
            other = call(second_halves_body, row(chips * part), chips)(*held)
        other = swap(other, 1)
        own, reply = experts(
            held + [other], [part] * chips + [chips * part], [chips * part, chips * part]
        )
        back = swap(reply, 1)
        if part % 16:
            joined = [
                jnp.concatenate([a[m * part : (m + 1) * part] for a in (own, back)], axis=0)
                for m in range(chips)
            ]
        else:
            joined = call(join_body, (block,) * chips, 2)(own, back)
        got_back = [joined[0]] + [swap(joined[m], CORES * m) for m in range(1, chips)]
        if block.shape[0] % 16:
            got_back = [jnp.concatenate(got_back, axis=0)]
        got_back = call(
            functools.partial(gather_body, sources=sources),
            (row(half),) * sources,
            sources + len(got_back),
        )(*[metas[d] for d in chunk], *got_back)
        for d, total in zip(chunk, got_back):
            sums[d] = swap(total, d * plane) if d else total
    return call(combine_body, sds((1, tokens, width), BF16), GROUPS + 2)(*sums, hidden, dest_cols)


def solution(mesh):
    return jax.shard_map(
        on_device,
        mesh=mesh,
        in_specs=(
            P("dp", "sp", None),
            P("dp", "sp", None),
            P("dp", "sp", None),
            P("dp", "sp", None),
            P("dp", "sp", None),
            P(),
            P(),
            P(),
            P(),
            P("dp", "sp", None),
            P("dp", "sp", None),
            P(("sp", "dp"), None, None),
            P(("sp", "dp"), None, None),
            P(("sp", "dp"), None, None),
        ),
        out_specs=P("dp", "sp", None),
        check_vma=False,
    )
```

```python
import functools
import math

import jax
import jax.numpy as jnp
from jax import lax
from jax.experimental import pallas as pl
from jax.experimental.pallas import tpu as pltpu
from jax.sharding import PartitionSpec as P


HD = 64
GROUPS = 4
CORES = 2
CHUNKS = ((2,), (3,), (1,), (0,))
norm_eps = 1e-05
F32 = jnp.float32
BF16 = jnp.bfloat16
MB = 1024 * 1024
FLOPS = 1.5e7
BYTES = 3.0e6

VM = pl.BlockSpec(memory_space=pltpu.VMEM)
SM = pl.BlockSpec(memory_space=pltpu.SMEM)
HB = pl.BlockSpec(memory_space=pltpu.HBM)
NT = (((1,), (1,)), ((), ()))


def call(body, out, n_in, scratch=(), limit=8, in_specs=None, us=1.0):
    return pl.pallas_call(
        body,
        out_shape=out,
        in_specs=in_specs or [VM] * n_in,
        out_specs=jax.tree.map(lambda _: VM, out),
        scratch_shapes=list(scratch),
        compiler_params=pltpu.CompilerParams(vmem_limit_bytes=limit * MB),
        cost_estimate=pl.CostEstimate(flops=int(us * FLOPS), bytes_accessed=int(us * BYTES), transcendentals=0),
    )


def in_hbm(array):
    return pltpu.with_memory_space_constraint(array, pltpu.HBM)


def iota(shape, dim):
    return lax.broadcasted_iota(jnp.int32, shape, dim)


def pack_body(q_ref, k_ref, v_ref, ks_ref, out_ref):
    n, rows, cols = out_ref.shape
    tokens, heads = ks_ref.shape[1], ks_ref.shape[2]
    local = heads // n
    pieces = tokens // cols
    eye = (iota((heads, heads), 0) == iota((heads, heads), 1)).astype(BF16)
    shift = lax.dot_general(eye, ks_ref[0], NT, preferred_element_type=F32)
    pad = rows - 3 * tokens
    for d in range(n):
        lanes = slice(d * cols, (d + 1) * cols)
        out_ref[d, 0:tokens, :] = q_ref[0, :, lanes]
        out_ref[d, tokens : 2 * tokens, :] = k_ref[0, :, lanes]
        out_ref[d, 2 * tokens : 3 * tokens, :] = v_ref[0, :, lanes]
        tail = [
            shift[d * local + h : d * local + h + 1, p * cols : (p + 1) * cols]
            for h in range(local)
            for p in range(pieces)
        ]
        tail.append(jnp.zeros((pad - len(tail), cols), F32))
        out_ref[d, 3 * tokens :, :] = jnp.concatenate(tail, axis=0).astype(BF16)


def pick_body(me_ref, q_ref, k_ref, v_ref, ks_ref, route_ref, rw_ref, *refs, plane, cap):
    out_refs, (line_ref, table_ref, meta_ref) = refs[:-8], refs[-8:-5]
    ks_in, route_in, rw_in, sems, small_sems = refs[-5:]
    small = [
        pltpu.make_async_copy(source, target, small_sems.at[i])
        for i, (source, target) in enumerate(
            ((ks_ref, ks_in), (route_ref, route_in), (rw_ref, rw_in))
        )
    ]
    for copy in small:
        copy.start()
    _, cols = out_refs[0].shape
    heads, tokens = ks_in.shape[1], ks_in.shape[2]
    local = heads // len(out_refs)
    step = len(out_refs) // GROUPS
    copies = []
    for k, out_ref in enumerate(out_refs):
        lanes = pl.ds(pl.multiple_of((me_ref[1] ^ k) * cols, cols), cols)
        for part, ref in enumerate((q_ref, k_ref, v_ref)):
            copies.append(
                pltpu.make_async_copy(
                    ref.at[0, :, lanes],
                    out_ref.at[part * tokens : (part + 1) * tokens, :],
                    sems.at[k, part],
                )
            )
    for copy in copies:
        copy.start()
    for copy in small:
        copy.wait()
    line_ref[...], table_ref[...], metas = routing(me_ref, route_in[0], rw_in[0], plane, cap)
    meta_ref[...] = metas[0]
    line, head = iota((8, heads), 0), iota((8, heads), 1)
    for k, out_ref in enumerate(out_refs):
        take = (head == line + (me_ref[1] ^ k) * local) & (line < local)
        shift = jnp.dot(take.astype(F32).astype(BF16), ks_in[0], preferred_element_type=F32)
        out_ref[3 * tokens : 3 * tokens + 8, :] = shift.astype(BF16)
        out_ref[3 * tokens + 8 :, :] = (
            metas[k // step] if k % step == 0 else jnp.zeros((8, cols), BF16)
        )
    for copy in copies:
        copy.wait()


def fetch_body(*refs):
    half = len(refs) // 2
    copies = [
        pltpu.make_async_copy(source, target, refs[-1].at[i])
        for i, (source, target) in enumerate(zip(refs[:half], refs[half : 2 * half]))
    ]
    for copy in copies:
        copy.start()
    for copy in copies:
        copy.wait()


def attend(me_ref, hs_ref, x_ref, scratch, row_at, key_at, count, diagonal, carries):
    z_ref, b_ref, w_ref = scratch
    cols = x_ref.shape[2]
    tokens = z_ref.shape[1]
    local, pieces = cols // HD, tokens // cols
    span = count * tokens
    lane = iota((tokens, cols), 1) // HD
    keys = x_ref[pl.ds(key_at, count), tokens : 2 * tokens, :].reshape(span, cols)
    values = x_ref[pl.ds(key_at, count), 2 * tokens : 3 * tokens, :].reshape(span, cols)
    row, col = iota((2 * tokens, 2 * tokens), 0), iota((2 * tokens, 2 * tokens), 1)
    summing = jnp.where((col >= tokens) | (row % tokens >= col), 1.0, 0.0).astype(BF16)
    causal = iota((tokens, tokens), 1) < iota((tokens, tokens), 0)
    for h in range(local):
        q = x_ref[row_at, 0:tokens, :].astype(F32) * (1.0 / math.sqrt(HD))
        q = jnp.where(lane == h, q, 0.0).astype(BF16)
        logits = lax.dot_general(q, keys, NT, preferred_element_type=F32)
        base = 3 * tokens + h * pieces
        for j in range(count):
            at = slice(j * tokens, (j + 1) * tokens)
            off = [x_ref[key_at + j, base + p : base + p + 1, :] for p in range(pieces)]
            off = off[0] if pieces == 1 else jnp.concatenate(off, axis=1)
            z = logits[:, at] + (off.astype(F32) + hs_ref[me_ref[1] * local + h])
            z_ref[h, :, at] = z
            breaks = -(jnp.maximum(z, 0.0) + jnp.log(1.0 + jnp.exp(-jnp.abs(z))))
            if diagonal and j == count - 1:
                breaks = jnp.where(causal, breaks, 0.0)
            high = breaks.astype(BF16)
            tile = slice((h * count + j) * tokens, (h * count + j + 1) * tokens)
            b_ref[tile, 0:tokens] = high
            b_ref[tile, tokens:] = (breaks - high.astype(F32)).astype(BF16)
    sums = jnp.dot(b_ref[0 : local * span, :], summing, preferred_element_type=F32)
    total, totals = None, []
    for h in range(local):
        carry = carries[h] if carries else None
        for j in range(count - 1, -1, -1):
            at = slice(j * tokens, (j + 1) * tokens)
            tile = slice((h * count + j) * tokens, (h * count + j + 1) * tokens)
            power = z_ref[h, :, at] + sums[tile, 0:tokens]
            if carry is not None:
                power = power + carry
            weight = jnp.exp(power)
            if diagonal and j == count - 1:
                weight = jnp.where(causal, weight, 0.0)
            w_ref[h, :, at] = weight.astype(BF16)
            part = sums[tile, tokens:]
            carry = part if carry is None else carry + part
        totals.append(carry)
        got = jnp.dot(w_ref[h, :, 0:span], values, preferred_element_type=F32)
        total = got if total is None else jnp.where(lane == h, got, total)
    return total, totals


def near_body(me_ref, hs_ref, *refs):
    x_refs, (part_ref, carry_ref, x_ref), scratch = refs[:-6], refs[-6:-3], refs[-3:]
    half = len(x_refs)
    for k, ref in enumerate(x_refs):
        x_ref[(me_ref[1] & (half - 1)) ^ k] = ref[...]
    for i in range(half):
        total, totals = attend(me_ref, hs_ref, x_ref, scratch, i, 0, i + 1, True, None)
        part_ref[i] = total
        for h, carry in enumerate(totals):
            carry_ref[i, h] = carry


def attention_body(me_ref, hs_ref, near_ref, near_carry_ref, *refs):
    x_refs, (out_ref, x_ref, part_ref, carry_ref), scratch = refs[:-7], refs[-7:-3], refs[-3:]
    n = len(x_refs)
    half = n // 2
    for k, ref in enumerate(x_refs):
        x_ref[me_ref[1] ^ k] = ref[...]
    mine = me_ref[1] & half
    other = mine ^ half
    for i in range(half):
        part_ref[mine + i] = near_ref[i]
        carry_ref[mine + i] = near_carry_ref[i]
    for i in range(half):
        total, totals = attend(
            me_ref, hs_ref, x_ref, scratch, other + i, other, i + 1, True, None
        )
        part_ref[other + i] = total
        for h, carry in enumerate(totals):
            carry_ref[other + i, h] = carry
    for i in range(half):
        out_ref[i] = part_ref[i].astype(BF16)
    for i in range(half, n):
        carries = [carry_ref[i, h] for h in range(carry_ref.shape[1])]
        total, _ = attend(me_ref, hs_ref, x_ref, scratch, i, 0, half, False, carries)
        out_ref[i] = (part_ref[i] + total).astype(BF16)


def routing(me_ref, route, weights, plane, cap):
    tokens = route.shape[1]
    bits = plane.bit_length() - 1
    zme, pme = me_ref[0] >> bits, me_ref[0] & (plane - 1)
    eye = iota((tokens, tokens), 0) == iota((tokens, tokens), 1)
    before = (iota((tokens, tokens), 0) < iota((tokens, tokens), 1)).astype(BF16)

    def to_col(line):
        return jnp.sum(jnp.where(eye, line, 0.0), axis=1, keepdims=True)

    def count(hot):
        return jnp.dot(hot.astype(BF16), before, preferred_element_type=F32)

    chosen = [route[k : k + 1].astype(F32) for k in range(2)]
    names = iota((GROUPS * plane, tokens), 0).astype(F32)
    hot = [(names == e).astype(F32) for e in chosen]
    earlier = count(hot[0] + hot[1])
    ranks = [jnp.sum(h * earlier, axis=0, keepdims=True) for h in hot]
    group = route[0:1] >> bits
    in_group = (iota((8, tokens), 0) == group).astype(F32)
    place = jnp.sum(in_group * count(in_group), axis=0, keepdims=True)
    lines = [jnp.where(group == (zme ^ d), place, -1.0) for d in range(GROUPS)]
    cols = [to_col(line) for line in lines]
    lane = iota((tokens, 128), 1)
    table = jnp.zeros((tokens, 128), F32)
    for k, c in enumerate(cols):
        table = jnp.where(lane == k, c, table)
    relay = [
        to_col((((route[k : k + 1] & (plane - 1)) ^ pme) * cap).astype(F32) + ranks[k])
        for k in range(2)
    ]
    shares = [to_col(weights[k : k + 1]) for k in range(2)]
    slot = iota((tokens, tokens), 1).astype(F32)
    metas = []
    for c in cols:
        pick = slot == c

        def gathered(column):
            return jnp.sum(jnp.where(pick, column, 0.0), axis=0, keepdims=True)

        out = [gathered(v + 1.0) - 1.0 for v in relay]
        for share in shares:
            rest = gathered(share)
            for _ in range(3):
                term = rest.astype(BF16).astype(F32)
                out.append(term)
                rest = rest - term
        metas.append(jnp.concatenate(out, axis=0).astype(BF16))
    lines = jnp.concatenate(lines + [jnp.zeros((4, tokens), F32)], axis=0)
    return lines.astype(jnp.int32), table.astype(jnp.int32), metas


def route_body(me_ref, route_ref, rw_ref, line_ref, table_ref, *meta_refs, plane, cap):
    line_ref[...], table_ref[...], metas = routing(
        me_ref, route_ref[0], rw_ref[0], plane, cap
    )
    for ref, meta in zip(meta_refs, metas):
        ref[...] = meta


def hidden_body(att_ref, stream_ref, mg_ref, w_ref, pg_ref, dest_ref, hid_ref, *far_refs):
    n, tokens, cols = att_ref.shape
    pieces = [att_ref[s].astype(F32) for s in range(n)]
    if cols % 128 == 0:
        pieces = [jnp.concatenate(pieces, axis=1)]
    size = pieces[0].shape[1]
    square = sum(jnp.sum(p * p, axis=1, keepdims=True) for p in pieces)
    scale = lax.rsqrt(square / (n * cols) + norm_eps)
    mixed = None
    for s, p in enumerate(pieces):
        at = slice(s * size, (s + 1) * size)
        normed = (p * scale * mg_ref[:, at]).astype(BF16)
        part = jnp.dot(normed, w_ref[at, :], preferred_element_type=F32)
        mixed = part if mixed is None else mixed + part
    summed = stream_ref[0].astype(F32) + mixed
    mean = jnp.mean(summed * summed, axis=1, keepdims=True)
    hidden = (summed * lax.rsqrt(mean + norm_eps) * pg_ref[...]).astype(BF16)
    hid_ref[...] = hidden
    for d, ref in enumerate(far_refs):
        pick = iota((ref.shape[0], tokens), 0) == dest_ref[d : d + 1, :]
        ref[...] = jnp.dot(
            pick.astype(F32).astype(BF16), hidden, preferred_element_type=F32
        ).astype(BF16)


def meta_of(ref):
    return ref[ref.shape[0] - 8 :].astype(F32)


def relay_body(*refs, sources):
    x_refs, meta_refs, out_refs = refs[:sources], refs[sources : 2 * sources], refs[2 * sources :]
    half = x_refs[0].shape[0]
    block = out_refs[0].shape[0]
    slot = iota((block * len(out_refs), half), 0)
    rows = None
    for x_ref, meta_ref in zip(x_refs, meta_refs):
        place = meta_of(meta_ref)[0:2, 0:half].astype(jnp.int32)
        pick = (slot == place[0:1]) | (slot == place[1:2])
        part = jnp.dot(pick.astype(F32).astype(BF16), x_ref[...], preferred_element_type=F32)
        rows = part if rows is None else rows + part
    rows = rows.astype(BF16)
    for m, ref in enumerate(out_refs):
        ref[...] = rows[m * block : (m + 1) * block]


def expert_body(*refs, takes):
    x_refs, (wg_ref, wu_ref, wd_ref), out_refs = (
        refs[: len(takes)],
        refs[len(takes) : len(takes) + 3],
        refs[len(takes) + 3 :],
    )
    parts = [ref[0:take] for ref, take in zip(x_refs, takes)]
    x = parts[0] if len(parts) == 1 else jnp.concatenate(parts, axis=0)
    gate = jnp.dot(x, wg_ref[0], preferred_element_type=F32)
    upper = jnp.dot(x, wu_ref[0], preferred_element_type=F32)
    inner = (gate / (1.0 + jnp.exp(-gate)) * upper).astype(BF16)
    out = jnp.dot(inner, wd_ref[0], preferred_element_type=F32).astype(BF16)
    at = 0
    for ref in out_refs:
        ref[...] = out[at : at + ref.shape[0]]
        at += ref.shape[0]


def second_halves_body(*refs):
    out_ref = refs[-1]
    part = out_ref.shape[0] // (len(refs) - 1)
    for m, ref in enumerate(refs[:-1]):
        out_ref[m * part : (m + 1) * part] = ref[part:]


def join_body(own_ref, back_ref, *out_refs):
    part = out_refs[0].shape[0] // 2
    for m, ref in enumerate(out_refs):
        at = slice(m * part, (m + 1) * part)
        ref[0:part] = own_ref[at]
        ref[part:] = back_ref[at]


def gather_body(*refs, sources):
    meta_refs, row_refs, out_refs = refs[:sources], refs[sources:-sources], refs[-sources:]
    parts = [ref[...] for ref in row_refs]
    rows = parts[0] if len(parts) == 1 else jnp.concatenate(parts, axis=0)
    for meta_ref, out_ref in zip(meta_refs, out_refs):
        half = out_ref.shape[0]
        eye = iota((half, half), 0) == iota((half, half), 1)
        slot = iota((half, rows.shape[0]), 1).astype(F32)
        meta = meta_of(meta_ref)[:, 0:half]
        total = None
        for k in range(2):
            share = meta[2 + 3 * k : 3 + 3 * k]
            for r in range(3 + 3 * k, 5 + 3 * k):
                share = share + meta[r : r + 1]
            place, weight = [
                jnp.sum(jnp.where(eye, line, 0.0), axis=1, keepdims=True)
                for line in (meta[k : k + 1], share)
            ]
            pick = (slot == place).astype(F32).astype(BF16)
            part = jnp.dot(pick, rows, preferred_element_type=F32) * weight
            total = part if total is None else total + part
        out_ref[...] = total.astype(BF16)


def gathered_body(*refs, first):
    far_refs, (hid_ref, dest_ref, out_ref) = refs[:-3], refs[-3:]
    tokens = hid_ref.shape[0]
    result = hid_ref[...].astype(F32)
    for d, ref in enumerate(far_refs, first):
        slot = iota((tokens, ref.shape[0]), 1)
        hot = (slot == dest_ref[:, d : d + 1]).astype(F32).astype(BF16)
        result = result + jnp.dot(hot, ref[...], preferred_element_type=F32)
    out_ref[...] = result.astype(out_ref.dtype).reshape(out_ref.shape)


def on_device(
    stream,
    queries,
    keys_in,
    values_in,
    key_shift,
    head_shift,
    mix_gain,
    out_weight,
    post_gain,
    route,
    route_weight,
    w_gate,
    w_up,
    w_down,
):
    tokens, width = stream.shape[1], stream.shape[2]
    size_sp, size_dp = lax.axis_size("sp"), lax.axis_size("dp")
    heads = key_shift.shape[2]
    local = heads // size_sp
    cols = queries.shape[2] // size_sp
    rows = 3 * tokens + 16
    n_expert = size_sp * size_dp
    plane = n_expert // GROUPS
    chips = plane // CORES
    cap = tokens // plane
    half = tokens // 2
    both = ("sp", "dp")
    sds = jax.ShapeDtypeStruct
    sp = lax.axis_index("sp")
    me = jnp.stack([sp * size_dp + lax.axis_index("dp"), sp]).astype(jnp.int32)

    def swap(array, bit):
        return lax.ppermute(array, both, [(i, i ^ bit) for i in range(n_expert)])

    routes = (route.swapaxes(1, 2), route_weight.swapaxes(1, 2))
    tables = (sds((8, tokens), jnp.int32), sds((tokens, 128), jnp.int32))
    ranked = dict(plane=plane, cap=cap)
    inside = cols == tokens
    if inside:
        *sent, dest_rows, dest_cols, meta = call(
            functools.partial(pick_body, **ranked),
            (sds((rows, cols), BF16),) * size_sp + tables + (sds((8, tokens), BF16),),
            0,
            in_specs=[SM] + [HB] * 6,
            scratch=[
                pltpu.VMEM((1, heads, tokens), BF16),
                pltpu.VMEM((1, 2, tokens), jnp.int32),
                pltpu.VMEM((1, 2, tokens), F32),
                pltpu.SemaphoreType.DMA((size_sp, 3)),
                pltpu.SemaphoreType.DMA((3,)),
            ],
        )(me, *map(in_hbm, (queries, keys_in, values_in, key_shift.swapaxes(1, 2)) + routes))
    else:
        sent = call(pack_body, sds((size_sp, rows, cols), BF16), 4)(
            queries, keys_in, values_in, key_shift
        )
        sent = [
            lax.dynamic_index_in_dim(sent, sp ^ k, 0, keepdims=False) for k in range(size_sp)
        ]
    got = [sent[0]] + [None] * (size_sp - 1)
    for k in range(size_sp - 1, 0, -1):
        got[k] = swap(sent[k], k * size_dp)
    if inside:
        metas = [meta] + [got[d * size_sp // GROUPS] for d in range(1, GROUPS)]
    else:
        dest_rows, dest_cols, *metas = call(
            functools.partial(route_body, **ranked),
            tables + (sds((8, tokens), BF16),) * GROUPS,
            3,
            in_specs=[SM, VM, VM],
        )(me, *routes)
        for d in range(1, GROUPS):
            metas[d] = swap(metas[d], d * plane)
    later = [in_hbm(x) for x in (out_weight, stream, mix_gain[None], post_gain[None], w_down)]
    out_weight, stream, mix_gain, post_gain, w_down = call(
        fetch_body,
        tuple(sds(x.shape, x.dtype) for x in later),
        0,
        in_specs=[HB] * len(later),
        scratch=[pltpu.SemaphoreType.DMA((len(later),))],
        us=5,
    )(*later)
    halved = size_sp // 2
    scratch = [
        pltpu.VMEM((local, tokens, halved * tokens), F32),
        pltpu.VMEM((local * halved * tokens, 2 * tokens), BF16),
        pltpu.VMEM((local, tokens, halved * tokens), BF16),
    ]
    near = call(
        near_body,
        (sds((halved, tokens, cols), F32), sds((halved, local, tokens, tokens), F32)),
        0,
        in_specs=[SM, SM] + [VM] * halved,
        scratch=[pltpu.VMEM((halved, rows, cols), BF16)] + scratch,
        us=2,
    )(me, head_shift, *got[:halved])
    att = call(
        attention_body,
        sds((size_sp, tokens, cols), BF16),
        0,
        in_specs=[SM, SM] + [VM] * (2 + size_sp),
        scratch=[
            pltpu.VMEM((size_sp, rows, cols), BF16),
            pltpu.VMEM((size_sp, tokens, cols), F32),
            pltpu.VMEM((size_sp, local, tokens, tokens), F32),
        ]
        + scratch,
        us=6,
        limit=12,
    )(me, head_shift, *near, *got)
    att = lax.all_to_all(att, "sp", split_axis=0, concat_axis=0, tiled=True)
    row = lambda count: sds((count, width), BF16)
    hidden, *far = call(
        hidden_body, (row(tokens),) + (row(half),) * GROUPS, 6, us=2
    )(att, stream, mix_gain, out_weight, post_gain, dest_rows)
    for d in range(1, GROUPS):
        far[d] = swap(far[d], d * plane)

    def experts(pieces, takes, outs):
        if any(take % 8 for take in takes):
            pieces = [jnp.concatenate([p[:t] for p, t in zip(pieces, takes)], axis=0)]
            takes = [sum(takes)]
        return call(
            functools.partial(expert_body, takes=takes),
            tuple(row(o) for o in outs),
            len(takes) + 3,
            limit=8,
            us=0.02 * sum(takes),
        )(*pieces, w_gate, w_up, w_down)

    sums = [None] * GROUPS
    for chunk in CHUNKS:
        sources = len(chunk)
        block = row(CORES * cap * sources)
        part = cap * sources
        blocks = call(
            functools.partial(relay_body, sources=sources), (block,) * chips, 2 * sources
        )(*[far[d] for d in chunk], *[metas[d] for d in chunk])
        held = [blocks[0]] + [
            swap(blocks[m], CORES * m) for m in range(chips - 1, 0, -1)
        ][::-1]
        if part % 16:
            other = jnp.concatenate([b[part:] for b in held], axis=0)
        else:
            other = call(second_halves_body, row(chips * part), chips)(*held)
        other = swap(other, 1)
        own, reply = experts(
            held + [other], [part] * chips + [chips * part], [chips * part, chips * part]
        )
        back = swap(reply, 1)
        if part % 16:
            joined = [
                jnp.concatenate([a[m * part : (m + 1) * part] for a in (own, back)], axis=0)
                for m in range(chips)
            ]
        else:
            joined = call(join_body, (block,) * chips, 2)(own, back)
        got_back = [joined[0]] + [swap(joined[m], CORES * m) for m in range(chips - 1, 0, -1)][::-1]
        if block.shape[0] % 16:
            got_back = [jnp.concatenate(got_back, axis=0)]
        got_back = call(
            functools.partial(gather_body, sources=sources),
            (row(half),) * sources,
            sources + len(got_back),
        )(*[metas[d] for d in chunk], *got_back)
        for d, total in zip(chunk, got_back):
            sums[d] = swap(total, d * plane) if d else total
    partly = call(
        functools.partial(gathered_body, first=0), sds((tokens, width), F32), GROUPS + 1
    )(*sums[:-1], hidden, dest_cols)
    return call(
        functools.partial(gathered_body, first=GROUPS - 1), sds((1, tokens, width), BF16), 3
    )(sums[-1], partly, dest_cols)


def solution(mesh):
    return jax.shard_map(
        on_device,
        mesh=mesh,
        in_specs=(
            P("dp", "sp", None),
            P("dp", "sp", None),
            P("dp", "sp", None),
            P("dp", "sp", None),
            P("dp", "sp", None),
            P(),
            P(),
            P(),
            P(),
            P("dp", "sp", None),
            P("dp", "sp", None),
            P(("sp", "dp"), None, None),
            P(("sp", "dp"), None, None),
            P(("sp", "dp"), None, None),
        ),
        out_specs=P("dp", "sp", None),
        check_vma=False,
    )
```

```python
import functools
import math

import jax
import jax.numpy as jnp
from jax import lax
from jax.experimental import pallas as pl
from jax.experimental.pallas import tpu as pltpu
from jax.sharding import PartitionSpec as P


HD = 64
GROUPS = 4
CORES = 2
EARLY, LATE = (0, 2), (1, 3)
CHUNKS = ((2,), (3,), (1,), (0,))
norm_eps = 1e-05
F32 = jnp.float32
BF16 = jnp.bfloat16
MB = 1024 * 1024
FLOPS = 1.5e7
BYTES = 3.0e6

VM = pl.BlockSpec(memory_space=pltpu.VMEM)
SM = pl.BlockSpec(memory_space=pltpu.SMEM)
HB = pl.BlockSpec(memory_space=pltpu.HBM)
NT = (((1,), (1,)), ((), ()))


def call(body, out, n_in, scratch=(), limit=8, in_specs=None, us=1.0):
    return pl.pallas_call(
        body,
        out_shape=out,
        in_specs=in_specs or [VM] * n_in,
        out_specs=jax.tree.map(lambda _: VM, out),
        scratch_shapes=list(scratch),
        compiler_params=pltpu.CompilerParams(vmem_limit_bytes=limit * MB),
        cost_estimate=pl.CostEstimate(flops=int(us * FLOPS), bytes_accessed=int(us * BYTES), transcendentals=0),
    )


def in_hbm(array):
    return pltpu.with_memory_space_constraint(array, pltpu.HBM)


def iota(shape, dim):
    return lax.broadcasted_iota(jnp.int32, shape, dim)


def pack_body(q_ref, k_ref, v_ref, ks_ref, out_ref):
    n, rows, cols = out_ref.shape
    tokens, heads = ks_ref.shape[1], ks_ref.shape[2]
    local = heads // n
    pieces = tokens // cols
    eye = (iota((heads, heads), 0) == iota((heads, heads), 1)).astype(BF16)
    shift = lax.dot_general(eye, ks_ref[0], NT, preferred_element_type=F32)
    pad = rows - 3 * tokens
    for d in range(n):
        lanes = slice(d * cols, (d + 1) * cols)
        out_ref[d, 0:tokens, :] = q_ref[0, :, lanes]
        out_ref[d, tokens : 2 * tokens, :] = k_ref[0, :, lanes]
        out_ref[d, 2 * tokens : 3 * tokens, :] = v_ref[0, :, lanes]
        tail = [
            shift[d * local + h : d * local + h + 1, p * cols : (p + 1) * cols]
            for h in range(local)
            for p in range(pieces)
        ]
        tail.append(jnp.zeros((pad - len(tail), cols), F32))
        out_ref[d, 3 * tokens :, :] = jnp.concatenate(tail, axis=0).astype(BF16)


def pick_body(me_ref, q_ref, k_ref, v_ref, ks_ref, route_ref, rw_ref, *refs, plane, cap):
    out_refs, (line_ref, table_ref, meta_ref) = refs[:-8], refs[-8:-5]
    ks_in, route_in, rw_in, sems, small_sems = refs[-5:]
    small = [
        pltpu.make_async_copy(source, target, small_sems.at[i])
        for i, (source, target) in enumerate(
            ((ks_ref, ks_in), (route_ref, route_in), (rw_ref, rw_in))
        )
    ]
    for copy in small:
        copy.start()
    _, cols = out_refs[0].shape
    heads, tokens = ks_in.shape[1], ks_in.shape[2]
    local = heads // len(out_refs)
    step = len(out_refs) // GROUPS
    copies = []
    for k, out_ref in enumerate(out_refs):
        lanes = pl.ds(pl.multiple_of((me_ref[1] ^ k) * cols, cols), cols)
        for part, ref in enumerate((q_ref, k_ref, v_ref)):
            copies.append(
                pltpu.make_async_copy(
                    ref.at[0, :, lanes],
                    out_ref.at[part * tokens : (part + 1) * tokens, :],
                    sems.at[k, part],
                )
            )
    for copy in copies:
        copy.start()
    for copy in small:
        copy.wait()
    line_ref[...], table_ref[...], metas = routing(me_ref, route_in[0], rw_in[0], plane, cap)
    meta_ref[...] = metas[0]
    line, head = iota((8, heads), 0), iota((8, heads), 1)
    for k, out_ref in enumerate(out_refs):
        take = (head == line + (me_ref[1] ^ k) * local) & (line < local)
        shift = jnp.dot(take.astype(F32).astype(BF16), ks_in[0], preferred_element_type=F32)
        out_ref[3 * tokens : 3 * tokens + 8, :] = shift.astype(BF16)
        out_ref[3 * tokens + 8 :, :] = (
            metas[k // step] if k % step == 0 else jnp.zeros((8, cols), BF16)
        )
    for copy in copies:
        copy.wait()


def fetch_body(*refs):
    half = len(refs) // 2
    copies = [
        pltpu.make_async_copy(source, target, refs[-1].at[i])
        for i, (source, target) in enumerate(zip(refs[:half], refs[half : 2 * half]))
    ]
    for copy in copies:
        copy.start()
    for copy in copies:
        copy.wait()


def attend(me_ref, hs_ref, x_ref, scratch, row_at, key_at, count, diagonal, carries):
    z_ref, b_ref, w_ref = scratch
    cols = x_ref.shape[2]
    tokens = z_ref.shape[1]
    local, pieces = cols // HD, tokens // cols
    span = count * tokens
    lane = iota((tokens, cols), 1) // HD
    keys = x_ref[pl.ds(key_at, count), tokens : 2 * tokens, :].reshape(span, cols)
    values = x_ref[pl.ds(key_at, count), 2 * tokens : 3 * tokens, :].reshape(span, cols)
    row, col = iota((2 * tokens, 2 * tokens), 0), iota((2 * tokens, 2 * tokens), 1)
    summing = jnp.where((col >= tokens) | (row % tokens >= col), 1.0, 0.0).astype(BF16)
    causal = iota((tokens, tokens), 1) < iota((tokens, tokens), 0)
    for h in range(local):
        q = x_ref[row_at, 0:tokens, :].astype(F32) * (1.0 / math.sqrt(HD))
        q = jnp.where(lane == h, q, 0.0).astype(BF16)
        logits = lax.dot_general(q, keys, NT, preferred_element_type=F32)
        base = 3 * tokens + h * pieces
        for j in range(count):
            at = slice(j * tokens, (j + 1) * tokens)
            off = [x_ref[key_at + j, base + p : base + p + 1, :] for p in range(pieces)]
            off = off[0] if pieces == 1 else jnp.concatenate(off, axis=1)
            z = logits[:, at] + (off.astype(F32) + hs_ref[me_ref[1] * local + h])
            z_ref[h, :, at] = z
            breaks = -(jnp.maximum(z, 0.0) + jnp.log(1.0 + jnp.exp(-jnp.abs(z))))
            if diagonal and j == count - 1:
                breaks = jnp.where(causal, breaks, 0.0)
            high = breaks.astype(BF16)
            tile = slice((h * count + j) * tokens, (h * count + j + 1) * tokens)
            b_ref[tile, 0:tokens] = high
            b_ref[tile, tokens:] = (breaks - high.astype(F32)).astype(BF16)
    sums = jnp.dot(b_ref[0 : local * span, :], summing, preferred_element_type=F32)
    total, totals = None, []
    for h in range(local):
        carry = carries[h] if carries else None
        for j in range(count - 1, -1, -1):
            at = slice(j * tokens, (j + 1) * tokens)
            tile = slice((h * count + j) * tokens, (h * count + j + 1) * tokens)
            power = z_ref[h, :, at] + sums[tile, 0:tokens]
            if carry is not None:
                power = power + carry
            weight = jnp.exp(power)
            if diagonal and j == count - 1:
                weight = jnp.where(causal, weight, 0.0)
            w_ref[h, :, at] = weight.astype(BF16)
            part = sums[tile, tokens:]
            carry = part if carry is None else carry + part
        totals.append(carry)
        got = jnp.dot(w_ref[h, :, 0:span], values, preferred_element_type=F32)
        total = got if total is None else jnp.where(lane == h, got, total)
    return total, totals


def near_body(me_ref, hs_ref, *refs):
    x_refs, (part_ref, carry_ref, x_ref), scratch = refs[:-6], refs[-6:-3], refs[-3:]
    half = len(x_refs)
    for k, ref in enumerate(x_refs):
        x_ref[(me_ref[1] & (half - 1)) ^ k] = ref[...]
    for i in range(half):
        total, totals = attend(me_ref, hs_ref, x_ref, scratch, i, 0, i + 1, True, None)
        part_ref[i] = total
        for h, carry in enumerate(totals):
            carry_ref[i, h] = carry


def attention_body(me_ref, hs_ref, near_ref, near_carry_ref, *refs):
    x_refs, (out_ref, x_ref, part_ref, carry_ref), scratch = refs[:-7], refs[-7:-3], refs[-3:]
    n = len(x_refs)
    half = n // 2
    for k, ref in enumerate(x_refs):
        x_ref[me_ref[1] ^ k] = ref[...]
    mine = me_ref[1] & half
    other = mine ^ half
    for i in range(half):
        part_ref[mine + i] = near_ref[i]
        carry_ref[mine + i] = near_carry_ref[i]
    for i in range(half):
        total, totals = attend(
            me_ref, hs_ref, x_ref, scratch, other + i, other, i + 1, True, None
        )
        part_ref[other + i] = total
        for h, carry in enumerate(totals):
            carry_ref[other + i, h] = carry
    for i in range(half):
        out_ref[i] = part_ref[i].astype(BF16)
    for i in range(half, n):
        carries = [carry_ref[i, h] for h in range(carry_ref.shape[1])]
        total, _ = attend(me_ref, hs_ref, x_ref, scratch, i, 0, half, False, carries)
        out_ref[i] = (part_ref[i] + total).astype(BF16)


def routing(me_ref, route, weights, plane, cap):
    tokens = route.shape[1]
    bits = plane.bit_length() - 1
    zme, pme = me_ref[0] >> bits, me_ref[0] & (plane - 1)
    eye = iota((tokens, tokens), 0) == iota((tokens, tokens), 1)
    before = (iota((tokens, tokens), 0) < iota((tokens, tokens), 1)).astype(BF16)

    def to_col(line):
        return jnp.sum(jnp.where(eye, line, 0.0), axis=1, keepdims=True)

    def count(hot):
        return jnp.dot(hot.astype(BF16), before, preferred_element_type=F32)

    chosen = [route[k : k + 1].astype(F32) for k in range(2)]
    names = iota((GROUPS * plane, tokens), 0).astype(F32)
    hot = [(names == e).astype(F32) for e in chosen]
    earlier = count(hot[0] + hot[1])
    ranks = [jnp.sum(h * earlier, axis=0, keepdims=True) for h in hot]
    group = route[0:1] >> bits
    in_group = (iota((8, tokens), 0) == group).astype(F32)
    place = jnp.sum(in_group * count(in_group), axis=0, keepdims=True)
    lines = [jnp.where(group == (zme ^ d), place, -1.0) for d in range(GROUPS)]
    cols = [to_col(line) for line in lines]
    lane = iota((tokens, 128), 1)
    table = jnp.zeros((tokens, 128), F32)
    for k, c in enumerate(cols):
        table = jnp.where(lane == k, c, table)
    relay = [
        to_col((((route[k : k + 1] & (plane - 1)) ^ pme) * cap).astype(F32) + ranks[k])
        for k in range(2)
    ]
    shares = [to_col(weights[k : k + 1]) for k in range(2)]
    slot = iota((tokens, tokens), 1).astype(F32)
    metas = []
    for c in cols:
        pick = slot == c

        def gathered(column):
            return jnp.sum(jnp.where(pick, column, 0.0), axis=0, keepdims=True)

        out = [gathered(v + 1.0) - 1.0 for v in relay]
        for share in shares:
            rest = gathered(share)
            for _ in range(3):
                term = rest.astype(BF16).astype(F32)
                out.append(term)
                rest = rest - term
        metas.append(jnp.concatenate(out, axis=0).astype(BF16))
    lines = jnp.concatenate(lines + [jnp.zeros((4, tokens), F32)], axis=0)
    return lines.astype(jnp.int32), table.astype(jnp.int32), metas


def route_body(me_ref, route_ref, rw_ref, line_ref, table_ref, *meta_refs, plane, cap):
    line_ref[...], table_ref[...], metas = routing(
        me_ref, route_ref[0], rw_ref[0], plane, cap
    )
    for ref, meta in zip(meta_refs, metas):
        ref[...] = meta


def hidden_body(att_ref, stream_ref, mg_ref, w_ref, pg_ref, dest_ref, hid_ref, *far_refs):
    n, tokens, cols = att_ref.shape
    pieces = [att_ref[s].astype(F32) for s in range(n)]
    if cols % 128 == 0:
        pieces = [jnp.concatenate(pieces, axis=1)]
    size = pieces[0].shape[1]
    square = sum(jnp.sum(p * p, axis=1, keepdims=True) for p in pieces)
    scale = lax.rsqrt(square / (n * cols) + norm_eps)
    mixed = None
    for s, p in enumerate(pieces):
        at = slice(s * size, (s + 1) * size)
        normed = (p * scale * mg_ref[:, at]).astype(BF16)
        part = jnp.dot(normed, w_ref[at, :], preferred_element_type=F32)
        mixed = part if mixed is None else mixed + part
    summed = stream_ref[0].astype(F32) + mixed
    mean = jnp.mean(summed * summed, axis=1, keepdims=True)
    hidden = (summed * lax.rsqrt(mean + norm_eps) * pg_ref[...]).astype(BF16)
    hid_ref[...] = hidden
    for d, ref in enumerate(far_refs):
        pick = iota((ref.shape[0], tokens), 0) == dest_ref[d : d + 1, :]
        ref[...] = jnp.dot(
            pick.astype(F32).astype(BF16), hidden, preferred_element_type=F32
        ).astype(BF16)


def meta_of(ref):
    return ref[ref.shape[0] - 8 :].astype(F32)


def relay_body(*refs, sources):
    x_refs, meta_refs, out_refs = refs[:sources], refs[sources : 2 * sources], refs[2 * sources :]
    half = x_refs[0].shape[0]
    block = out_refs[0].shape[0]
    slot = iota((block * len(out_refs), half), 0)
    rows = None
    for x_ref, meta_ref in zip(x_refs, meta_refs):
        place = meta_of(meta_ref)[0:2, 0:half].astype(jnp.int32)
        pick = (slot == place[0:1]) | (slot == place[1:2])
        part = jnp.dot(pick.astype(F32).astype(BF16), x_ref[...], preferred_element_type=F32)
        rows = part if rows is None else rows + part
    rows = rows.astype(BF16)
    for m, ref in enumerate(out_refs):
        ref[...] = rows[m * block : (m + 1) * block]


def expert_body(*refs, takes):
    x_refs, (wg_ref, wu_ref, wd_ref), out_refs = (
        refs[: len(takes)],
        refs[len(takes) : len(takes) + 3],
        refs[len(takes) + 3 :],
    )
    parts = [ref[0:take] for ref, take in zip(x_refs, takes)]
    x = parts[0] if len(parts) == 1 else jnp.concatenate(parts, axis=0)
    gate = jnp.dot(x, wg_ref[0], preferred_element_type=F32)
    upper = jnp.dot(x, wu_ref[0], preferred_element_type=F32)
    inner = (gate / (1.0 + jnp.exp(-gate)) * upper).astype(BF16)
    out = jnp.dot(inner, wd_ref[0], preferred_element_type=F32).astype(BF16)
    at = 0
    for ref in out_refs:
        ref[...] = out[at : at + ref.shape[0]]
        at += ref.shape[0]


def second_halves_body(*refs):
    out_ref = refs[-1]
    part = out_ref.shape[0] // (len(refs) - 1)
    for m, ref in enumerate(refs[:-1]):
        out_ref[m * part : (m + 1) * part] = ref[part:]


def join_body(own_ref, back_ref, *out_refs):
    part = out_refs[0].shape[0] // 2
    for m, ref in enumerate(out_refs):
        at = slice(m * part, (m + 1) * part)
        ref[0:part] = own_ref[at]
        ref[part:] = back_ref[at]


def gather_body(*refs, sources):
    meta_refs, row_refs, out_refs = refs[:sources], refs[sources:-sources], refs[-sources:]
    parts = [ref[...] for ref in row_refs]
    rows = parts[0] if len(parts) == 1 else jnp.concatenate(parts, axis=0)
    for meta_ref, out_ref in zip(meta_refs, out_refs):
        half = out_ref.shape[0]
        eye = iota((half, half), 0) == iota((half, half), 1)
        slot = iota((half, rows.shape[0]), 1).astype(F32)
        meta = meta_of(meta_ref)[:, 0:half]
        total = None
        for k in range(2):
            share = meta[2 + 3 * k : 3 + 3 * k]
            for r in range(3 + 3 * k, 5 + 3 * k):
                share = share + meta[r : r + 1]
            place, weight = [
                jnp.sum(jnp.where(eye, line, 0.0), axis=1, keepdims=True)
                for line in (meta[k : k + 1], share)
            ]
            pick = (slot == place).astype(F32).astype(BF16)
            part = jnp.dot(pick, rows, preferred_element_type=F32) * weight
            total = part if total is None else total + part
        out_ref[...] = total.astype(BF16)


def gathered_body(*refs, chosen):
    far_refs, (hid_ref, dest_ref, out_ref) = refs[:-3], refs[-3:]
    tokens = hid_ref.shape[0]
    result = hid_ref[...].astype(F32)
    for d, ref in zip(chosen, far_refs):
        slot = iota((tokens, ref.shape[0]), 1)
        hot = (slot == dest_ref[:, d : d + 1]).astype(F32).astype(BF16)
        result = result + jnp.dot(hot, ref[...], preferred_element_type=F32)
    out_ref[...] = result.astype(out_ref.dtype).reshape(out_ref.shape)


def on_device(
    stream,
    queries,
    keys_in,
    values_in,
    key_shift,
    head_shift,
    mix_gain,
    out_weight,
    post_gain,
    route,
    route_weight,
    w_gate,
    w_up,
    w_down,
):
    tokens, width = stream.shape[1], stream.shape[2]
    size_sp, size_dp = lax.axis_size("sp"), lax.axis_size("dp")
    heads = key_shift.shape[2]
    local = heads // size_sp
    cols = queries.shape[2] // size_sp
    rows = 3 * tokens + 16
    n_expert = size_sp * size_dp
    plane = n_expert // GROUPS
    chips = plane // CORES
    cap = tokens // plane
    half = tokens // 2
    both = ("sp", "dp")
    sds = jax.ShapeDtypeStruct
    sp = lax.axis_index("sp")
    me = jnp.stack([sp * size_dp + lax.axis_index("dp"), sp]).astype(jnp.int32)

    def swap(array, bit):
        return lax.ppermute(array, both, [(i, i ^ bit) for i in range(n_expert)])

    routes = (route.swapaxes(1, 2), route_weight.swapaxes(1, 2))
    tables = (sds((8, tokens), jnp.int32), sds((tokens, 128), jnp.int32))
    ranked = dict(plane=plane, cap=cap)
    inside = cols == tokens
    if inside:
        *sent, dest_rows, dest_cols, meta = call(
            functools.partial(pick_body, **ranked),
            (sds((rows, cols), BF16),) * size_sp + tables + (sds((8, tokens), BF16),),
            0,
            in_specs=[SM] + [HB] * 6,
            scratch=[
                pltpu.VMEM((1, heads, tokens), BF16),
                pltpu.VMEM((1, 2, tokens), jnp.int32),
                pltpu.VMEM((1, 2, tokens), F32),
                pltpu.SemaphoreType.DMA((size_sp, 3)),
                pltpu.SemaphoreType.DMA((3,)),
            ],
        )(me, *map(in_hbm, (queries, keys_in, values_in, key_shift.swapaxes(1, 2)) + routes))
    else:
        sent = call(pack_body, sds((size_sp, rows, cols), BF16), 4)(
            queries, keys_in, values_in, key_shift
        )
        sent = [
            lax.dynamic_index_in_dim(sent, sp ^ k, 0, keepdims=False) for k in range(size_sp)
        ]
    got = [sent[0]] + [None] * (size_sp - 1)
    for k in range(size_sp - 1, 0, -1):
        got[k] = swap(sent[k], k * size_dp)
    if inside:
        metas = [meta] + [got[d * size_sp // GROUPS] for d in range(1, GROUPS)]
    else:
        dest_rows, dest_cols, *metas = call(
            functools.partial(route_body, **ranked),
            tables + (sds((8, tokens), BF16),) * GROUPS,
            3,
            in_specs=[SM, VM, VM],
        )(me, *routes)
        for d in range(1, GROUPS):
            metas[d] = swap(metas[d], d * plane)
    later = [in_hbm(x) for x in (out_weight, stream, mix_gain[None], post_gain[None], w_down)]
    out_weight, stream, mix_gain, post_gain, w_down = call(
        fetch_body,
        tuple(sds(x.shape, x.dtype) for x in later),
        0,
        in_specs=[HB] * len(later),
        scratch=[pltpu.SemaphoreType.DMA((len(later),))],
        us=5,
    )(*later)
    halved = size_sp // 2
    scratch = [
        pltpu.VMEM((local, tokens, halved * tokens), F32),
        pltpu.VMEM((local * halved * tokens, 2 * tokens), BF16),
        pltpu.VMEM((local, tokens, halved * tokens), BF16),
    ]
    near = call(
        near_body,
        (sds((halved, tokens, cols), F32), sds((halved, local, tokens, tokens), F32)),
        0,
        in_specs=[SM, SM] + [VM] * halved,
        scratch=[pltpu.VMEM((halved, rows, cols), BF16)] + scratch,
        us=2,
    )(me, head_shift, *got[:halved])
    att = call(
        attention_body,
        sds((size_sp, tokens, cols), BF16),
        0,
        in_specs=[SM, SM] + [VM] * (2 + size_sp),
        scratch=[
            pltpu.VMEM((size_sp, rows, cols), BF16),
            pltpu.VMEM((size_sp, tokens, cols), F32),
            pltpu.VMEM((size_sp, local, tokens, tokens), F32),
        ]
        + scratch,
        us=6,
        limit=12,
    )(me, head_shift, *near, *got)
    att = lax.all_to_all(att, "sp", split_axis=0, concat_axis=0, tiled=True)
    row = lambda count: sds((count, width), BF16)
    hidden, *far = call(
        hidden_body, (row(tokens),) + (row(half),) * GROUPS, 6, us=2
    )(att, stream, mix_gain, out_weight, post_gain, dest_rows)
    for d in range(1, GROUPS):
        far[d] = swap(far[d], d * plane)

    def experts(pieces, takes, outs):
        if any(take % 8 for take in takes):
            pieces = [jnp.concatenate([p[:t] for p, t in zip(pieces, takes)], axis=0)]
            takes = [sum(takes)]
        return call(
            functools.partial(expert_body, takes=takes),
            tuple(row(o) for o in outs),
            len(takes) + 3,
            limit=8,
            us=0.02 * sum(takes),
        )(*pieces, w_gate, w_up, w_down)

    sums = [None] * GROUPS
    for chunk in CHUNKS:
        sources = len(chunk)
        block = row(CORES * cap * sources)
        part = cap * sources
        blocks = call(
            functools.partial(relay_body, sources=sources), (block,) * chips, 2 * sources
        )(*[far[d] for d in chunk], *[metas[d] for d in chunk])
        held = [blocks[0]] + [
            swap(blocks[m], CORES * m) for m in range(chips - 1, 0, -1)
        ][::-1]
        if part % 16:
            other = jnp.concatenate([b[part:] for b in held], axis=0)
        else:
            other = call(second_halves_body, row(chips * part), chips)(*held)
        other = swap(other, 1)
        own, reply = experts(
            held + [other], [part] * chips + [chips * part], [chips * part, chips * part]
        )
        back = swap(reply, 1)
        if part % 16:
            joined = [
                jnp.concatenate([a[m * part : (m + 1) * part] for a in (own, back)], axis=0)
                for m in range(chips)
            ]
        else:
            joined = call(join_body, (block,) * chips, 2)(own, back)
        got_back = [joined[0]] + [swap(joined[m], CORES * m) for m in range(chips - 1, 0, -1)][::-1]
        if block.shape[0] % 16:
            got_back = [jnp.concatenate(got_back, axis=0)]
        got_back = call(
            functools.partial(gather_body, sources=sources),
            (row(half),) * sources,
            sources + len(got_back),
        )(*[metas[d] for d in chunk], *got_back)
        for d, total in zip(chunk, got_back):
            sums[d] = swap(total, d * plane) if d else total
    partly = call(
        functools.partial(gathered_body, chosen=EARLY), sds((tokens, width), F32), len(EARLY) + 2
    )(*[sums[d] for d in EARLY], hidden, dest_cols)
    return call(
        functools.partial(gathered_body, chosen=LATE), sds((1, tokens, width), BF16), len(LATE) + 2
    )(*[sums[d] for d in LATE], partly, dest_cols)


def solution(mesh):
    return jax.shard_map(
        on_device,
        mesh=mesh,
        in_specs=(
            P("dp", "sp", None),
            P("dp", "sp", None),
            P("dp", "sp", None),
            P("dp", "sp", None),
            P("dp", "sp", None),
            P(),
            P(),
            P(),
            P(),
            P("dp", "sp", None),
            P("dp", "sp", None),
            P(("sp", "dp"), None, None),
            P(("sp", "dp"), None, None),
            P(("sp", "dp"), None, None),
        ),
        out_specs=P("dp", "sp", None),
        check_vma=False,
    )
```
